512 devices in a mesh: fs: 16 (over y, x), tp: 32 (over z, core).
Axes of the slice: x: 4, y: 4, z: 16, core: 2. Of those that a mesh axis runs over, the one named last changes fastest.
Arguments:
- tokens: bfloat16 [65536, 2048], P(('fs', 'tp')), may hold values from -6 to 6
- gain: float32 [2048], P('fs'), may hold values from 0.1 to 1.9
- ex_gate: float32 [32, 256, 2048], P('tp', None, 'fs'), may hold values from -0.125 to 0.125
- ex_up: float32 [32, 256, 2048], P('tp', None, 'fs'), may hold values from -0.125 to 0.125
- ex_down: float32 [32, 256, 2048], P('tp', None, 'fs'), may hold values from -0.375 to 0.375
- sh_gate: float32 [512, 2048], P('tp', 'fs'), may hold values from -0.125 to 0.125
- sh_up: float32 [512, 2048], P('tp', 'fs'), may hold values from -0.125 to 0.125
- sh_down: float32 [512, 2048], P('tp', 'fs'), may hold values from -0.25 to 0.25
- routes: int32 [65536, 4], P(('fs', 'tp')), may hold values from 0 to 31, all different within a row; in each aligned block of 128 rows (0 to 127, 128 to 255, ...) at most 18 rows name the same one
- route_weight: float32 [65536, 4], P(('fs', 'tp')), may hold values from 0.1 to 1
Outputs:
- mixed: bfloat16 [65536, 2048], P(('fs', 'tp'))
- expert_gate: bfloat16 [32, 256, 2048], P('tp')
- expert_up: bfloat16 [32, 256, 2048], P('tp')
- expert_down: bfloat16 [32, 256, 2048], P('tp')
- shared_gate: bfloat16 [512, 2048], P('tp')
- shared_up: bfloat16 [512, 2048], P('tp')
- shared_down: bfloat16 [512, 2048], P('tp')
The draws below stay inside these ranges and needn't reach their ends.
Inputs may be any that keep to these rules, and one draw needn't show every extreme that they name: `routes`: each row names 4 different experts. Among the rows of one device no expert is named by more than 18 rows, and in every draw some expert is named by exactly 18 rows of some device.
All inputs are finite; a program needn't handle non-finite values.
Results may differ from the reference program's by a relative error of at most 0.0085.
Values may be sent and summed in bfloat16 or wider, within the bound.
No kernel may reach another device: no remote copies, remote signals or barrier semaphores. Data moves between devices by JAX's collectives and lax.ppermute only.
A program may use at most 64 MiB of HBM per device.

```python
import math
import jax
import jax.numpy as jnp
import numpy as np
from jax import lax

D = 2048
FF_EXPERT = 256
FF_SHARED = 512
TOP = 4
TOK_DEV = 128
EXPERTS = 32
CAP = 18
TOKENS = 65536


def steps_of(own_key, shape, split, smallest, top_value):
    loudness, own = 1.0, jax.random.fold_in(own_key, 6)
    for dim, shards_of in split:
        heights = jnp.exp(jax.random.uniform(jax.random.fold_in(own, dim), (shards_of,), jnp.float32, smallest / len(split), top_value / len(split)))
        loudness = loudness * jnp.repeat(heights, shape[dim] // shards_of).reshape([-1 if axis == dim else 1 for axis in range(len(shape))])
    return loudness


def routed_block(rng, own, number, rows, count, top, most, skew):
    order = jax.random.permutation(rng, count)
    packed, ordinary = load_shares(count, rows * top, most, skew, True), load_shares(count, rows * top, most, skew, False)
    places = jnp.arange(count)

    def named(tallies, turn):
        used = int((tallies > 0).sum())
        fixed = max(1, used // 4)
        passed = fixed + (places - fixed + turn * (used - fixed)) % max(1, count - fixed)
        return jnp.zeros((count,), jnp.int32).at[order[jnp.where(places < fixed, places, passed)]].set(jnp.asarray(tallies, jnp.int32))

    tallies = jnp.where(number % 4 == 0, named(packed, number // 4), named(ordinary, number - number // 4 - 1))
    mixed = jax.random.permutation(jax.random.fold_in(own, 3), count)
    giver, taker = mixed[0:count // 2 * 2:2], mixed[1:count // 2 * 2:2]
    margin = jnp.minimum(tallies[giver] - 1, most - tallies[taker]) // 2
    margin = jnp.where((giver == order[0]) | (taker == order[0]) | (tallies[taker] == 0), 0, jnp.maximum(margin, 0))
    passed = jax.random.randint(jax.random.fold_in(own, 4), (count // 2,), 0, 1 << 20) % (margin + 1)
    tallies = tallies.at[giver].add(-passed).at[taker].add(passed)
    labels = jnp.searchsorted(jnp.cumsum(tallies), jnp.arange(rows * top), side="right").astype(jnp.int32)
    listing = labels.reshape(top, rows).T
    listing = listing[jax.random.permutation(jax.random.fold_in(own, 1), rows)]
    turn = jax.random.randint(jax.random.fold_in(own, 2), (rows, 1), 0, top)
    return jnp.take_along_axis(listing, (jnp.arange(top)[None, :] + turn) % top, axis=1)


def load_shares(number_of, total, bound, skew, full):
    loads = [(1 << 20) // math.isqrt(grade ** skew) + 1 for grade in range(1, number_of + 1)]
    largest = bound if full else min(bound, max(-(-total // number_of), total * loads[0] // sum(loads)))
    least = 1 if total - largest >= number_of - 1 else 0
    given, rest = [largest] + [least] * (number_of - 1), total - largest - least * (number_of - 1)
    while rest > 0:
        movable = [i for i in range(1, number_of) if given[i] < largest] or [i for i in range(1, number_of) if given[i] < bound]
        whole, remaining = sum([loads[i] for i in movable]), rest
        for i in movable:
            more = min(bound - given[i], max(1, remaining * loads[i] // whole), rest)
            given[i] = given[i] + more
            rest = rest - more
    return np.array(given)


def normal_values(key, shape, spread, bound, pieces=(), kind=jnp.bfloat16):
    values = spread * jax.random.normal(key, shape, jnp.float32)
    if pieces:
        values = values * steps_of(key, shape, pieces, -0.22, 0.18)
    return jnp.clip(values, -bound, bound).astype(kind)


def setup_inputs(seed: int = 0) -> dict:
    seeds = jax.random.split(jax.random.key(seed), 11)
    tokens = normal_values(seeds[0], (TOKENS, D), 1.0, 6.0, ((0, 512),))
    gain = jnp.clip(1.0 + 0.18 * jax.random.normal(seeds[1], (D,), jnp.float32), 0.1, 1.9)
    ex_gate = normal_values(seeds[2], (EXPERTS, FF_EXPERT, D), D ** -0.5, 0.125, ((0, 32), (2, 16)), jnp.float32)
    ex_up = normal_values(seeds[3], (EXPERTS, FF_EXPERT, D), D ** -0.5, 0.125, ((0, 32), (2, 16)), jnp.float32)
    ex_down = normal_values(seeds[4], (EXPERTS, FF_EXPERT, D), FF_EXPERT ** -0.5, 0.375, ((0, 32), (2, 16)), jnp.float32)
    sh_gate = normal_values(seeds[5], (FF_SHARED, D), D ** -0.5, 0.125, ((0, 32), (1, 16)), jnp.float32)
    sh_up = normal_values(seeds[6], (FF_SHARED, D), D ** -0.5, 0.125, ((0, 32), (1, 16)), jnp.float32)
    sh_down = normal_values(seeds[7], (FF_SHARED, D), FF_SHARED ** -0.5, 0.25, ((0, 32), (1, 16)), jnp.float32)
    routes_keys = jax.random.split(jax.random.fold_in(seeds[8], 1), TOKENS // TOK_DEV)
    routes_turns = jax.random.permutation(jax.random.fold_in(seeds[8], 3), TOKENS // TOK_DEV)
    routes = jax.vmap(lambda own, number: routed_block(jax.random.fold_in(seeds[8], 2), own, number, TOK_DEV, EXPERTS, TOP, CAP, 2))(routes_keys, routes_turns).reshape((TOKENS, TOP))
    route_weight = jnp.clip(jnp.exp(math.log(1.0) - 2.3025851 * jax.random.uniform(seeds[9], (TOKENS, TOP), jnp.float32) ** steps_of(seeds[9], (TOKENS, TOP), ((0, 512),), -0.2, 0.2)), 0.1, 1.0)
    return {"tokens": tokens, "gain": gain, "ex_gate": ex_gate, "ex_up": ex_up, "ex_down": ex_down, "sh_gate": sh_gate, "sh_up": sh_up, "sh_down": sh_down, "routes": routes, "route_weight": route_weight}


EPS = 1e-06
ROUTED_SCALE = 2.5
CONTRACT = (((1,), (1,)), ((), ()))

def against(row_block, weight):
    return lax.dot_general(row_block, weight, CONTRACT, preferred_element_type=jnp.float32)

def expert_apply(row_block, w_gate, w_up, w_down):
    hidden = (jax.nn.silu(against(row_block, w_gate)) * against(row_block, w_up)).astype(jnp.bfloat16)
    return jnp.dot(hidden, w_down, preferred_element_type=jnp.float32)

def slot_numbers(expert_ids, experts, capacity):
    flat_ids = expert_ids.reshape(-1).astype(jnp.int32)
    onehot = (flat_ids[:, None] == jnp.arange(experts, dtype=jnp.int32)[None, :]).astype(jnp.int32)
    before = jnp.cumsum(onehot, axis=0) - onehot
    ranking = lax.optimization_barrier(jnp.sum(before * onehot, axis=1)).astype(jnp.int32)
    return (flat_ids * capacity + ranking).astype(jnp.int32)

def reference(tokens, gain, ex_gate, ex_up, ex_down, sh_gate, sh_up, sh_down, routes, route_weight):
    scale = gain[None, :]
    expert_gate = (ex_gate * scale[None]).astype(jnp.bfloat16)
    expert_up = (ex_up * scale[None]).astype(jnp.bfloat16)
    expert_down = ex_down.astype(jnp.bfloat16)
    shared_gate = (sh_gate * scale).astype(jnp.bfloat16)
    shared_up = (sh_up * scale).astype(jnp.bfloat16)
    shared_down = sh_down.astype(jnp.bfloat16)
    values = tokens.astype(jnp.float32)
    normed = (values * lax.rsqrt(lax.optimization_barrier(jnp.mean(values * values, axis=1, keepdims=True)) + EPS)).astype(jnp.bfloat16)
    weights = route_weight / lax.optimization_barrier(jnp.sum(route_weight, axis=1, keepdims=True)) * ROUTED_SCALE
    blocks = TOKENS // TOK_DEV
    spots = jnp.arange(EXPERTS * CAP, dtype=jnp.int32)

    def one_block(inputs):
        row_block, expert_ids, block_weights = inputs
        shared = expert_apply(row_block, shared_gate, shared_up, shared_down)
        slots = slot_numbers(expert_ids, EXPERTS, CAP)
        placing = (spots[:, None] == slots[None, :]).astype(jnp.int32)
        placing = lax.optimization_barrier(jnp.sum(placing.reshape(EXPERTS * CAP, TOK_DEV, TOP), axis=2)).astype(jnp.bfloat16)
        outgoing = jnp.dot(placing, row_block, preferred_element_type=jnp.float32).astype(jnp.bfloat16)
        outgoing = outgoing.reshape(EXPERTS, CAP, D)

        def per_expert(parts):
            slot_rows, w_gate, w_up, w_down = parts
            return expert_apply(slot_rows, w_gate, w_up, w_down).astype(jnp.bfloat16)
        answered = lax.map(per_expert, (outgoing, expert_gate, expert_up, expert_down))
        picked = answered.reshape(EXPERTS * CAP, D)[slots].reshape(TOK_DEV, TOP, D)
        routed = lax.optimization_barrier(jnp.sum(block_weights[:, :, None] * picked.astype(jnp.float32), axis=1))
        return (shared + routed).astype(jnp.bfloat16)
    mixed = lax.map(one_block, (normed.reshape(blocks, TOK_DEV, D), routes.reshape(blocks, TOK_DEV, TOP), weights.reshape(blocks, TOK_DEV, TOP)))
    return (mixed.reshape(TOKENS, D), expert_gate, expert_up, expert_down, shared_gate, shared_up, shared_down)
```

```python
import functools

import jax
import jax.numpy as jnp
from jax import lax
from jax.experimental import pallas as pl
from jax.experimental.pallas import tpu as pltpu
from jax.sharding import Mesh
from jax.sharding import PartitionSpec as P

TP = ("tp_0", "tp_1")
PLANE = ("fs", "tp_1")
FS_TP = ("fs", "tp_0", "tp_1")

EPS = 1e-06
ROUTED_SCALE = 2.5
BF = jnp.bfloat16
F32 = jnp.float32
NT = (((1,), (1,)), ((), ()))

MAIN = 16
EXTRA = 2
QUARTERS = 4


def dot(a, b):
    return jnp.dot(a, b, preferred_element_type=F32)


def dot_nt(a, b):
    return lax.dot_general(a, b, NT, preferred_element_type=F32)


def iota(shape, dim):
    return lax.broadcasted_iota(jnp.int32, shape, dim)


def whole(shape):
    return pl.BlockSpec(shape, lambda: (0,) * len(shape))


def call(body, out, args, flops, name):
    moved = sum(a.size * a.dtype.itemsize for a in args) + sum(o.size * o.dtype.itemsize for o in out)
    return pl.pallas_call(
        body,
        out_shape=out,
        in_specs=[whole(a.shape) for a in args],
        out_specs=[whole(o.shape) for o in out],
        cost_estimate=pl.CostEstimate(flops=flops, bytes_accessed=moved, transcendentals=0),
        name=name,
    )(*args)


def fold_body(gain, eg, eu, ed, sg, su, sd, routed, both):
    scale = gain[...]
    rows = eg.shape[1]
    gate = (eg[0] * scale).astype(BF)
    up = (eu[0] * scale).astype(BF)
    down = ed[0].astype(BF)
    for i, part in enumerate((gate, up, down)):
        routed[i * rows : (i + 1) * rows, :] = part
        both[i * rows : (i + 1) * rows, :] = part
    at = 3 * rows
    few = sg.shape[0]
    for part in (sg[...] * scale, su[...] * scale, sd[...]):
        both[at : at + few, :] = part.astype(BF)
        at += few


def place_body(tokens, routes_t, outgoing, normed_out):
    values = tokens[...].astype(F32)
    mean = jnp.mean(values * values, axis=1, keepdims=True)
    normed = (values * lax.rsqrt(mean + EPS)).astype(BF)
    normed_out[...] = normed
    experts = outgoing.shape[0]
    top, rows = routes_t.shape
    ids = [routes_t[k : k + 1, :] for k in range(top)]
    hot = [(iota((experts, rows), 0) == ids[k]).astype(F32) for k in range(top)]
    named = sum(hot[1:], hot[0])
    earlier = (iota((rows, rows), 0) < iota((rows, rows), 1)).astype(BF)
    before = dot(named.astype(BF), earlier)
    ranks = [jnp.sum(before * h, axis=0, keepdims=True).astype(jnp.int32) for h in hot]
    spot = iota((experts * MAIN, rows), 0)
    main = jnp.zeros((experts * MAIN, rows), F32)
    for k in range(top):
        target = jnp.where(ranks[k] < MAIN, ids[k] * MAIN + ranks[k], -1)
        main = jnp.where(spot == target, 1.0, main)
    main = main.astype(BF)
    few = QUARTERS * EXTRA
    spot = iota((experts * few, rows), 0)
    part = normed.shape[1] // QUARTERS
    extra = jnp.zeros((experts * few, part), F32)
    for q in range(QUARTERS):
        piece = normed[:, q * part : (q + 1) * part]
        rows_q = dot(main, piece).astype(BF)
        outgoing[:, q * MAIN : (q + 1) * MAIN, :] = rows_q.reshape(experts, MAIN, part)
        pick = jnp.zeros((experts * few, rows), F32)
        for k in range(top):
            slot = ids[k] * few + q * EXTRA + ranks[k] - MAIN
            pick = jnp.where(spot == jnp.where(ranks[k] < MAIN, -1, slot), 1.0, pick)
        extra = extra + dot(pick.astype(BF), piece)
    outgoing[:, QUARTERS * MAIN :, :] = extra.reshape(experts, few, part).astype(BF)


def lanes(w, lo, hi, q, per):
    return jnp.concatenate([w[q * per + i, lo:hi, :] for i in range(per)], axis=1)


def expert_body(arrived, w, answered, acc_main, acc_extra, hid_main, hid_extra):
    sources = arrived.shape[0]
    part = arrived.shape[2]
    per = part // w.shape[2]
    width = w.shape[1] // 3
    few = QUARTERS * EXTRA
    tail = arrived[:, QUARTERS * MAIN :, :].astype(F32).reshape(sources * few, part).astype(BF)
    row = iota((sources * EXTRA, sources * few), 0)
    col = iota((sources * EXTRA, sources * few), 1)
    for q in range(QUARTERS):
        both = lanes(w, 0, 2 * width, q, per)
        x = arrived[:, q * MAIN : (q + 1) * MAIN, :].reshape(sources * MAIN, part)
        pick = (col == row // EXTRA * few + q * EXTRA + row % EXTRA).astype(F32).astype(BF)
        y = dot(pick, tail).astype(BF)
        if q == 0:
            acc_main[...] = dot_nt(x, both)
            acc_extra[...] = dot_nt(y, both)
        else:
            acc_main[...] += dot_nt(x, both)
            acc_extra[...] += dot_nt(y, both)
    for acc, hid in ((acc_main, hid_main), (acc_extra, hid_extra)):
        gate = acc[:, :width]
        hid[...] = (gate / (1.0 + jnp.exp(-gate)) * acc[:, width:]).astype(BF)
    row = iota((sources * few, sources * EXTRA), 0)
    col = iota((sources * few, sources * EXTRA), 1)
    back = jnp.zeros((sources * few, part), F32)
    for q in range(QUARTERS):
        down = lanes(w, 2 * width, 3 * width, q, per)
        out = dot(hid_main[...], down).astype(BF)
        answered[:, q * MAIN : (q + 1) * MAIN, :] = out.reshape(sources, MAIN, part)
        few_out = dot(hid_extra[...], down).astype(BF)
        put = (row == col // EXTRA * few + q * EXTRA + col % EXTRA).astype(F32).astype(BF)
        back = back + dot(put, few_out)
    answered[:, QUARTERS * MAIN :, :] = back.reshape(sources, few, part).astype(BF)


def shared_body(normed, w, out):
    devices, three, features = w.shape
    few = three // 3
    parts = [w[:, i * few : (i + 1) * few, :].reshape(devices * few, features) for i in range(3)]
    n = normed[...]
    gate = dot_nt(n, parts[0])
    up = dot_nt(n, parts[1])
    hidden = (gate / (1.0 + jnp.exp(-gate)) * up).astype(BF)
    out[...] = dot(hidden, parts[2])


def split_weight(w):
    high = w.astype(BF)
    return high, (w - high.astype(F32)).astype(BF)


def combine_body(returned, routes, route_weight, shared, mixed):
    experts = returned.shape[0]
    part = returned.shape[2]
    few = QUARTERS * EXTRA
    rows, top = routes.shape
    raw = route_weight[...]
    weights = raw / jnp.sum(raw, axis=1, keepdims=True) * ROUTED_SCALE
    ids = [routes[:, k : k + 1] for k in range(top)]
    hot = [(iota((rows, experts), 1) == ids[k]).astype(F32) for k in range(top)]
    named = sum(hot[1:], hot[0])
    earlier = (iota((rows, rows), 1) < iota((rows, rows), 0)).astype(BF)
    before = dot(earlier, named.astype(BF))
    ranks = [jnp.sum(before * h, axis=1, keepdims=True).astype(jnp.int32) for h in hot]
    spot = iota((rows, experts * MAIN), 1)
    main = jnp.zeros((rows, experts * MAIN), F32)
    for k in range(top):
        target = jnp.where(ranks[k] < MAIN, ids[k] * MAIN + ranks[k], -1)
        main = jnp.where(spot == target, weights[:, k : k + 1], main)
    high, low = split_weight(main)
    spot = iota((rows, experts * few), 1)
    tail = returned[:, QUARTERS * MAIN :, :].astype(F32).reshape(experts * few, part).astype(BF)
    for q in range(QUARTERS):
        x = returned[:, q * MAIN : (q + 1) * MAIN, :].reshape(experts * MAIN, part)
        pick = jnp.zeros((rows, experts * few), F32)
        for k in range(top):
            slot = ids[k] * few + q * EXTRA + ranks[k] - MAIN
            slot = jnp.where(ranks[k] < MAIN, -1, slot)
            pick = jnp.where(spot == slot, weights[:, k : k + 1], pick)
        pick_high, pick_low = split_weight(pick)
        routed = dot(high, x) + dot(low, x) + dot(pick_high, tail) + dot(pick_low, tail)
        at = slice(q * part, (q + 1) * part)
        mixed[:, at] = (shared[:, at] + routed).astype(BF)


def local(tokens, gain, ex_gate, ex_up, ex_down, sh_gate, sh_up, sh_down, routes, route_weight):
    rows, features = tokens.shape
    top = routes.shape[1]
    hidden, block = ex_gate.shape[1:]
    few = sh_gate.shape[0]
    parts = lax.axis_size("fs")
    experts = lax.axis_size(TP)
    part = features // QUARTERS
    shape = jax.ShapeDtypeStruct

    with jax.named_scope("fold"):
        args = (gain[None, :], ex_gate, ex_up, ex_down, sh_gate, sh_up, sh_down)
        out = (shape((3 * hidden, block), BF), shape((3 * hidden + 3 * few, block), BF))
        routed_w, both_w = call(fold_body, out, args, 10**6, "fold")
    with jax.named_scope("zgather"):
        over_z = lax.all_gather(routed_w, "tp_0", axis=0, tiled=False)
    with jax.named_scope("own"):
        copies = jnp.broadcast_to(both_w[None], (parts,) + both_w.shape)
        own = lax.all_to_all(copies, "fs", 0, 0, tiled=True)
    with jax.named_scope("place"):
        size = MAIN * QUARTERS + EXTRA * QUARTERS
        out = (shape((experts, size, part), BF), shape((rows, features), BF))
        flops = 2 * rows * features * experts * (MAIN + EXTRA)
        outgoing, normed = call(place_body, out, (tokens, routes.T), flops, "place")
    with jax.named_scope("send"):
        arrived = lax.all_to_all(outgoing, PLANE, 0, 0, tiled=True)
    with jax.named_scope("ownout"):
        own = jnp.moveaxis(own, 0, 1).reshape(-1, features)
        exp_gate, exp_up, exp_down = (own[i * hidden : (i + 1) * hidden][None] for i in range(3))
        shr = own[3 * hidden :]
        shr_gate, shr_up, shr_down = (shr[i * few : (i + 1) * few] for i in range(3))
    with jax.named_scope("shgather"):
        shared_w = lax.all_gather(shr, TP, axis=0, tiled=False)
    with jax.named_scope("weights"):
        expert_w = lax.all_to_all(over_z, "fs", 0, 0, tiled=True)
    with jax.named_scope("experts"):
        n = experts * MAIN
        m = experts * EXTRA
        out = shape(outgoing.shape, BF)
        answered = pl.pallas_call(
            expert_body,
            out_shape=out,
            in_specs=[whole(arrived.shape), whole(expert_w.shape)],
            out_specs=whole(out.shape),
            scratch_shapes=[
                pltpu.VMEM((n, 2 * hidden), F32),
                pltpu.VMEM((m, 2 * hidden), F32),
                pltpu.VMEM((n, hidden), BF),
                pltpu.VMEM((m, hidden), BF),
            ],
            cost_estimate=pl.CostEstimate(
                flops=6 * (n + m) * hidden * features, bytes_accessed=8 * 10**6, transcendentals=0
            ),
            name="experts",
        )(arrived, expert_w)
    with jax.named_scope("back"):
        returned = lax.all_to_all(answered, PLANE, 0, 0, tiled=True)
    with jax.named_scope("shared"):
        out = (shape((rows, features), F32),)
        (shared,) = call(shared_body, out, (normed, shared_w), 6 * rows * features * few * experts, "shared")
    with jax.named_scope("combine"):
        out = (shape((rows, features), BF),)
        args = (returned, routes, route_weight, shared)
        (mixed,) = call(combine_body, out, args, 4 * rows * features * (n + m), "combine")
    return (mixed, exp_gate, exp_up, exp_down, shr_gate, shr_up, shr_down)


def solution(mesh):
    split = Mesh(mesh.devices.reshape(mesh.shape["fs"], 16, 2), ("fs", "tp_0", "tp_1"))
    in_specs = (
        P(FS_TP, None),
        P("fs"),
        P(TP, None, "fs"),
        P(TP, None, "fs"),
        P(TP, None, "fs"),
        P(TP, "fs"),
        P(TP, "fs"),
        P(TP, "fs"),
        P(FS_TP, None),
        P(FS_TP, None),
    )
    out_specs = (
        P(FS_TP, None),
        P(TP, None, None),
        P(TP, None, None),
        P(TP, None, None),
        P(TP, None),
        P(TP, None),
        P(TP, None),
    )
    return jax.shard_map(local, mesh=split, in_specs=in_specs, out_specs=out_specs, check_vma=False)
```

```python
import jax
import jax.numpy as jnp
from jax import lax
from jax.experimental import pallas as pl
from jax.experimental.pallas import tpu as pltpu
from jax.sharding import Mesh
from jax.sharding import PartitionSpec as P


TP = ("tp_0", "tp_1")
FS = ("y", "x")
PLANE = FS + ("tp_1",)
FS_TP = FS + TP


EPS = 1e-06
ROUTED_SCALE = 2.5
BF = jnp.bfloat16
F32 = jnp.float32
NT = (((1,), (1,)), ((), ()))

MAIN = 16
EXTRA = 2
QUARTERS = 4
GRANT = 24 << 20


def dot(a, b):
    return jnp.dot(a, b, preferred_element_type=F32)


def dot_nt(a, b):
    return lax.dot_general(a, b, NT, preferred_element_type=F32)


def iota(shape, dim):
    return lax.broadcasted_iota(jnp.int32, shape, dim)


def whole(shape):
    return pl.BlockSpec(shape, lambda *_: (0,) * len(shape))


def call(body, out, args, flops, limit=None, specs=None, grid=(), scratch=()):
    moved = sum(a.size * a.dtype.itemsize for a in args) + sum(o.size * o.dtype.itemsize for o in out)
    return pl.pallas_call(
        body,
        grid=grid,
        out_shape=out,
        in_specs=specs or [whole(a.shape) for a in args],
        out_specs=[whole(o.shape) for o in out],
        scratch_shapes=list(scratch),
        cost_estimate=pl.CostEstimate(flops=flops, bytes_accessed=moved, transcendentals=0),
        compiler_params=pltpu.CompilerParams(vmem_limit_bytes=limit),
    )(*args)


def fold_body(gain, eg, eu, ed, sg, su, sd, routed, first, second):
    scale = gain[...]
    at = 0
    cut = second.shape[0]
    for part in (eg[0] * scale, eu[0] * scale, ed[0]):
        middle = part.shape[0] // 2
        for piece in (part[:middle].astype(BF), part[middle:].astype(BF)):
            rows = piece.shape[0]
            routed[at : at + rows, :] = piece
            if at < cut:
                first[at : at + rows, :] = piece
            else:
                second[at - cut : at - cut + rows, :] = piece
            at += rows
    at = cut
    for part in (sg[...] * scale, su[...] * scale, sd[...]):
        first[at : at + part.shape[0], :] = part.astype(BF)
        at += part.shape[0]


def place_body(tokens, routes_t, outgoing, normed_out):
    values = tokens[...].astype(F32)
    mean = jnp.mean(values * values, axis=1, keepdims=True)
    normed = (values * lax.rsqrt(mean + EPS)).astype(BF)
    normed_out[...] = normed
    experts = outgoing.shape[0]
    top, rows = routes_t.shape
    ids = [routes_t[k : k + 1, :] for k in range(top)]
    hot = [(iota((experts, rows), 0) == ids[k]).astype(F32) for k in range(top)]
    named = sum(hot[1:], hot[0])
    earlier = (iota((rows, rows), 0) < iota((rows, rows), 1)).astype(BF)
    before = dot(named.astype(BF), earlier)
    ranks = [jnp.sum(before * h, axis=0, keepdims=True).astype(jnp.int32) for h in hot]
    spot = iota((experts * MAIN, rows), 0)
    main = jnp.zeros((experts * MAIN, rows), F32)
    for k in range(top):
        target = jnp.where(ranks[k] < MAIN, ids[k] * MAIN + ranks[k], -1)
        main = jnp.where(spot == target, 1.0, main)
    main = main.astype(BF)
    few = QUARTERS * EXTRA
    spot = iota((experts * few, rows), 0)
    part = normed.shape[1] // QUARTERS
    extra = jnp.zeros((experts * few, part), F32)
    for q in range(QUARTERS):
        piece = normed[:, q * part : (q + 1) * part]
        rows_q = dot(main, piece).astype(BF)
        outgoing[:, q * MAIN : (q + 1) * MAIN, :] = rows_q.reshape(experts, MAIN, part)
        pick = jnp.zeros((experts * few, rows), F32)
        for k in range(top):
            slot = ids[k] * few + q * EXTRA + ranks[k] - MAIN
            pick = jnp.where(spot == jnp.where(ranks[k] < MAIN, -1, slot), 1.0, pick)
        extra = extra + dot(pick.astype(BF), piece)
    outgoing[:, QUARTERS * MAIN :, :] = extra.reshape(experts, few, part).astype(BF)


def lanes(w, lo, hi, q, per):
    return jnp.concatenate([w[q * per + i, lo:hi, :] for i in range(per)], axis=1)


def expert_body(arrived, w, answered, acc_main, acc_extra, hid_main, hid_extra):
    sources = arrived.shape[0]
    part = arrived.shape[2]
    per = part // w.shape[2]
    width = w.shape[1] // 3
    few = QUARTERS * EXTRA
    tail = arrived[:, QUARTERS * MAIN :, :].astype(F32).reshape(sources * few, part).astype(BF)
    row = iota((sources * EXTRA, sources * few), 0)
    col = iota((sources * EXTRA, sources * few), 1)
    for q in range(QUARTERS):
        both = lanes(w, 0, 2 * width, q, per)
        x = arrived[:, q * MAIN : (q + 1) * MAIN, :].reshape(sources * MAIN, part)
        pick = (col == row // EXTRA * few + q * EXTRA + row % EXTRA).astype(F32).astype(BF)
        y = dot(pick, tail).astype(BF)
        if q == 0:
            acc_main[...] = dot_nt(x, both)
            acc_extra[...] = dot_nt(y, both)
        else:
            acc_main[...] += dot_nt(x, both)
            acc_extra[...] += dot_nt(y, both)
    for acc, hid in ((acc_main, hid_main), (acc_extra, hid_extra)):
        gate = acc[:, :width]
        hid[...] = (gate / (1.0 + jnp.exp(-gate)) * acc[:, width:]).astype(BF)
    row = iota((sources * few, sources * EXTRA), 0)
    col = iota((sources * few, sources * EXTRA), 1)
    back = jnp.zeros((sources * few, part), F32)
    for q in range(QUARTERS):
        down = lanes(w, 2 * width, 3 * width, q, per)
        out = dot(hid_main[...], down).astype(BF)
        answered[:, q * MAIN : (q + 1) * MAIN, :] = out.reshape(sources, MAIN, part)
        few_out = dot(hid_extra[...], down).astype(BF)
        put = (row == col // EXTRA * few + q * EXTRA + col % EXTRA).astype(F32).astype(BF)
        back = back + dot(put, few_out)
    answered[:, QUARTERS * MAIN :, :] = back.reshape(sources, few, part).astype(BF)


def shared_body(normed, w, out):
    devices, three, features = w.shape
    few = three // 3
    parts = [w[:, i * few : (i + 1) * few, :].reshape(devices * few, features) for i in range(3)]
    n = normed[...]
    gate = dot_nt(n, parts[0])
    up = dot_nt(n, parts[1])
    hidden = (gate / (1.0 + jnp.exp(-gate)) * up).astype(BF)
    out[...] = dot(hidden, parts[2])


def split_weight(w):
    high = w.astype(BF)
    return high, (w - high.astype(F32)).astype(BF)


def mixers_body(routes, route_weight, main_high, main_low, few_high, few_low):
    rows, top = routes.shape
    few = QUARTERS * EXTRA
    experts = main_high.shape[1] // MAIN
    raw = route_weight[...]
    weights = raw / jnp.sum(raw, axis=1, keepdims=True) * ROUTED_SCALE
    ids = [routes[:, k : k + 1] for k in range(top)]
    hot = [(iota((rows, experts), 1) == ids[k]).astype(F32) for k in range(top)]
    named = sum(hot[1:], hot[0])
    earlier = (iota((rows, rows), 1) < iota((rows, rows), 0)).astype(BF)
    before = dot(earlier, named.astype(BF))
    ranks = [jnp.sum(before * h, axis=1, keepdims=True).astype(jnp.int32) for h in hot]
    spot = iota((rows, experts * MAIN), 1)
    main = jnp.zeros((rows, experts * MAIN), F32)
    for k in range(top):
        target = jnp.where(ranks[k] < MAIN, ids[k] * MAIN + ranks[k], -1)
        main = jnp.where(spot == target, weights[:, k : k + 1], main)
    main_high[...], main_low[...] = split_weight(main)
    spot = iota((rows, experts * few), 1)
    for q in range(QUARTERS):
        pick = jnp.zeros((rows, experts * few), F32)
        for k in range(top):
            slot = ids[k] * few + q * EXTRA + ranks[k] - MAIN
            slot = jnp.where(ranks[k] < MAIN, -1, slot)
            pick = jnp.where(spot == slot, weights[:, k : k + 1], pick)
        few_high[q], few_low[q] = split_weight(pick)


def combine_body(returned, main_high, main_low, few_high, few_low, shared_hbm, mixed, shared, sem):
    fetch = pltpu.make_async_copy(shared_hbm, shared, sem)
    fetch.start()
    experts = returned.shape[0]
    part = returned.shape[2]
    few = QUARTERS * EXTRA
    tail = returned[:, QUARTERS * MAIN :, :].astype(F32).reshape(experts * few, part).astype(BF)
    for q in range(QUARTERS):
        x = returned[:, q * MAIN : (q + 1) * MAIN, :].reshape(experts * MAIN, part)
        routed = dot(main_high[...], x) + dot(main_low[...], x)
        routed = routed + dot(few_high[q], tail) + dot(few_low[q], tail)
        if q == 0:
            fetch.wait()
        at = slice(q * part, (q + 1) * part)
        mixed[:, at] = (shared[:, at] + routed).astype(BF)


def swapped(array, axis, other):
    pairs = [(i, i ^ other) for i in range(lax.axis_size(axis))]
    return lax.ppermute(array, axis, pairs) if other else array


def place_of(index, other, block):
    return pl.ds(pl.multiple_of((index[0] ^ other) * block, block), block)


def few_body(index, *refs):
    stacks, out = refs[:-1], refs[-1]
    side, rows, block = stacks[0].shape
    for j, stack in enumerate(stacks):
        for k in range(side):
            out[:, place_of(index, j * side + k, block)] = stack[k, rows - out.shape[0] :, :]


def split_body(index, shr, *refs):
    outs = refs[-6:]
    side = (len(refs) - 6) // 2
    first, second = refs[:side], refs[side : 2 * side]
    gate, up, down = outs[:3]
    rows = gate.shape[1]
    half = rows // 2
    block = first[0].shape[2]
    for i in range(side):
        for j in range(side):
            at = place_of(index, i * side + j, block)
            gate[0, :, at] = first[i][j, :rows, :]
            up[0, :half, at] = first[i][j, rows : rows + half, :]
            up[0, half:, at] = second[j][i, :half, :]
            down[0, :, at] = second[j][i, half : half + rows, :]
    for i, ref in enumerate(outs[3:]):
        ref[...] = shr[i * ref.shape[0] : (i + 1) * ref.shape[0], :]


def step(tokens, gain, ex_gate, ex_up, ex_down, sh_gate, sh_up, sh_down, routes, route_weight):
    rows, features = tokens.shape
    hidden, block = ex_gate.shape[1:]
    few = sh_gate.shape[0]
    experts = lax.axis_size(TP)
    part = features // QUARTERS
    shape = jax.ShapeDtypeStruct

    args = (gain[None, :], ex_gate, ex_up, ex_down, sh_gate, sh_up, sh_down)
    cut = 3 * hidden // 2
    out = (shape((2 * cut, block), BF), shape((cut + 3 * few, block), BF), shape((cut, block), BF))
    routed_w, first_w, second_w = call(fold_body, out, args, 10**6)
    over_z = lax.all_gather(routed_w, "tp_0", axis=0, tiled=False)
    size = MAIN * QUARTERS + EXTRA * QUARTERS
    out = (shape((experts, size, part), BF), shape((rows, features), BF))
    flops = 2 * rows * features * experts * (MAIN + EXTRA)
    outgoing, normed = call(place_body, out, (tokens, routes.T), flops)
    arrived = lax.all_to_all(outgoing, PLANE, 0, 0, tiled=True)
    side = lax.axis_size("x")
    first = [swapped(first_w, "x", k) for k in range(side)]
    second = [swapped(second_w, "y", k) for k in range(side)]
    first, second = jnp.stack(first), jnp.stack(second)
    firsts = [swapped(first, "y", k) for k in range(side)]
    index = lax.axis_index(FS).astype(jnp.int32).reshape(1)
    scalar = [pl.BlockSpec(memory_space=pltpu.SMEM)]
    out = (shape((3 * few, features), BF),)
    specs = scalar + [whole(first.shape)] * side
    (shr,) = call(few_body, out, (index, *firsts), 10**6, None, specs)
    shared_w = lax.all_gather(shr, TP, axis=0, tiled=False)
    seconds = [swapped(second, "x", k) for k in range(side)]
    out = (shape((1, hidden, features), BF),) * 3 + (shape((few, features), BF),) * 3
    specs = scalar + [whole(shr.shape)] + [whole(first.shape)] * side + [whole(second.shape)] * side
    outs = call(split_body, out, (index, shr, *firsts, *seconds), 10**7, None, specs)
    expert_w = lax.all_to_all(over_z, FS, 0, 0, tiled=True)
    n = experts * MAIN
    m = experts * EXTRA
    out = shape(outgoing.shape, BF)
    answered = pl.pallas_call(
        expert_body,
        out_shape=out,
        in_specs=[whole(arrived.shape), whole(expert_w.shape)],
        out_specs=whole(out.shape),
        scratch_shapes=[
            pltpu.VMEM((n, 2 * hidden), F32),
            pltpu.VMEM((m, 2 * hidden), F32),
            pltpu.VMEM((n, hidden), BF),
            pltpu.VMEM((m, hidden), BF),
        ],
        cost_estimate=pl.CostEstimate(
            flops=6 * (n + m) * hidden * features, bytes_accessed=8 * 10**6, transcendentals=0
        ),
        compiler_params=pltpu.CompilerParams(vmem_limit_bytes=GRANT),
        name="experts",
    )(arrived, expert_w)
    returned = lax.all_to_all(answered, PLANE, 0, 0, tiled=True)
    out = (shape((rows, n), BF),) * 2 + (shape((QUARTERS, rows, m * QUARTERS), BF),) * 2
    mixers = call(mixers_body, out, (routes, route_weight), 10**7)
    out = (shape((rows, features), F32),)
    (shared,) = call(shared_body, out, (normed, shared_w), 6 * rows * features * few * experts)
    out = (shape((rows, features), BF),)
    args = (returned, *mixers, shared)
    specs = [whole(a.shape) for a in args[:-1]] + [pl.BlockSpec(memory_space=pltpu.HBM)]
    scratch = [pltpu.VMEM((rows, features), F32), pltpu.SemaphoreType.DMA(())]
    (mixed,) = call(
        combine_body, out, args, 4 * rows * features * (n + m), GRANT, specs, (), scratch
    )
    return (mixed, *outs)


def solution(mesh):
    split = Mesh(mesh.devices.reshape(4, 4, 16, 2), FS_TP)
    in_specs = (
        P(FS_TP, None),
        P(FS),
        P(TP, None, FS),
        P(TP, None, FS),
        P(TP, None, FS),
        P(TP, FS),
        P(TP, FS),
        P(TP, FS),
        P(FS_TP, None),
        P(FS_TP, None),
    )
    out_specs = (
        P(FS_TP, None),
        P(TP, None, None),
        P(TP, None, None),
        P(TP, None, None),
        P(TP, None),
        P(TP, None),
        P(TP, None),
    )
    return jax.shard_map(step, mesh=split, in_specs=in_specs, out_specs=out_specs, check_vma=False)
```

```python
import jax
import jax.numpy as jnp
from jax import lax
from jax.experimental import pallas as pl
from jax.experimental.pallas import tpu as pltpu
from jax.sharding import Mesh
from jax.sharding import PartitionSpec as P


TP = ("tp_0", "tp_1")
FS = ("y", "x")
PLANE = FS + ("tp_1",)
FS_TP = FS + TP


EPS = 1e-06
ROUTED_SCALE = 2.5
BF = jnp.bfloat16
F32 = jnp.float32
NT = (((1,), (1,)), ((), ()))

MAIN = 16
EXTRA = 2
QUARTERS = 4
GRANT = 24 << 20


def dot(a, b):
    return jnp.dot(a, b, preferred_element_type=F32)


def dot_nt(a, b):
    return lax.dot_general(a, b, NT, preferred_element_type=F32)


def iota(shape, dim):
    return lax.broadcasted_iota(jnp.int32, shape, dim)


def whole(shape):
    return pl.BlockSpec(shape, lambda *_: (0,) * len(shape))


def call(body, out, args, flops, limit=None, specs=None, grid=(), scratch=()):
    moved = sum(a.size * a.dtype.itemsize for a in args) + sum(o.size * o.dtype.itemsize for o in out)
    return pl.pallas_call(
        body,
        grid=grid,
        out_shape=out,
        in_specs=specs or [whole(a.shape) for a in args],
        out_specs=[whole(o.shape) for o in out],
        scratch_shapes=list(scratch),
        cost_estimate=pl.CostEstimate(flops=flops, bytes_accessed=moved, transcendentals=0),
        compiler_params=pltpu.CompilerParams(vmem_limit_bytes=limit),
    )(*args)


def fold_body(gain, eg, eu, ed, sg, su, sd, routed, first, second):
    scale = gain[...]
    at = 0
    cut = second.shape[0]
    for part in (eg[0] * scale, eu[0] * scale, ed[0]):
        middle = part.shape[0] // 2
        for piece in (part[:middle].astype(BF), part[middle:].astype(BF)):
            rows = piece.shape[0]
            routed[at : at + rows, :] = piece
            if at < cut:
                first[at : at + rows, :] = piece
            else:
                second[at - cut : at - cut + rows, :] = piece
            at += rows
    at = cut
    for part in (sg[...] * scale, su[...] * scale, sd[...]):
        first[at : at + part.shape[0], :] = part.astype(BF)
        at += part.shape[0]


def place_body(tokens, routes_t, outgoing, normed_out):
    values = tokens[...].astype(F32)
    mean = jnp.mean(values * values, axis=1, keepdims=True)
    normed = (values * lax.rsqrt(mean + EPS)).astype(BF)
    normed_out[...] = normed
    experts = outgoing.shape[0]
    top, rows = routes_t.shape
    ids = [routes_t[k : k + 1, :] for k in range(top)]
    hot = [(iota((experts, rows), 0) == ids[k]).astype(F32) for k in range(top)]
    named = sum(hot[1:], hot[0])
    earlier = (iota((rows, rows), 0) < iota((rows, rows), 1)).astype(BF)
    before = dot(named.astype(BF), earlier)
    ranks = [jnp.sum(before * h, axis=0, keepdims=True).astype(jnp.int32) for h in hot]
    spot = iota((experts * MAIN, rows), 0)
    main = jnp.zeros((experts * MAIN, rows), F32)
    for k in range(top):
        target = jnp.where(ranks[k] < MAIN, ids[k] * MAIN + ranks[k], -1)
        main = jnp.where(spot == target, 1.0, main)
    main = main.astype(BF)
    few = QUARTERS * EXTRA
    spot = iota((experts * few, rows), 0)
    part = normed.shape[1] // QUARTERS
    extra = jnp.zeros((experts * few, part), F32)
    for q in range(QUARTERS):
        piece = normed[:, q * part : (q + 1) * part]
        rows_q = dot(main, piece).astype(BF)
        outgoing[:, q * MAIN : (q + 1) * MAIN, :] = rows_q.reshape(experts, MAIN, part)
        pick = jnp.zeros((experts * few, rows), F32)
        for k in range(top):
            slot = ids[k] * few + q * EXTRA + ranks[k] - MAIN
            pick = jnp.where(spot == jnp.where(ranks[k] < MAIN, -1, slot), 1.0, pick)
        extra = extra + dot(pick.astype(BF), piece)
    outgoing[:, QUARTERS * MAIN :, :] = extra.reshape(experts, few, part).astype(BF)


def lanes(w, lo, hi, q, per):
    return jnp.concatenate([w[q * per + i, lo:hi, :] for i in range(per)], axis=1)


def expert_body(arrived, w, answered, acc_main, acc_extra, hid_main, hid_extra):
    sources = arrived.shape[0]
    part = arrived.shape[2]
    per = part // w.shape[2]
    width = w.shape[1] // 3
    few = QUARTERS * EXTRA
    tail = arrived[:, QUARTERS * MAIN :, :].astype(F32).reshape(sources * few, part).astype(BF)
    row = iota((sources * EXTRA, sources * few), 0)
    col = iota((sources * EXTRA, sources * few), 1)
    for q in range(QUARTERS):
        both = lanes(w, 0, 2 * width, q, per)
        x = arrived[:, q * MAIN : (q + 1) * MAIN, :].reshape(sources * MAIN, part)
        pick = (col == row // EXTRA * few + q * EXTRA + row % EXTRA).astype(F32).astype(BF)
        y = dot(pick, tail).astype(BF)
        if q == 0:
            acc_main[...] = dot_nt(x, both)
            acc_extra[...] = dot_nt(y, both)
        else:
            acc_main[...] += dot_nt(x, both)
            acc_extra[...] += dot_nt(y, both)
    for acc, hid in ((acc_main, hid_main), (acc_extra, hid_extra)):
        gate = acc[:, :width]
        hid[...] = (gate / (1.0 + jnp.exp(-gate)) * acc[:, width:]).astype(BF)
    row = iota((sources * few, sources * EXTRA), 0)
    col = iota((sources * few, sources * EXTRA), 1)
    back = jnp.zeros((sources * few, part), F32)
    for q in range(QUARTERS):
        down = lanes(w, 2 * width, 3 * width, q, per)
        out = dot(hid_main[...], down).astype(BF)
        answered[:, q * MAIN : (q + 1) * MAIN, :] = out.reshape(sources, MAIN, part)
        few_out = dot(hid_extra[...], down).astype(BF)
        put = (row == col // EXTRA * few + q * EXTRA + col % EXTRA).astype(F32).astype(BF)
        back = back + dot(put, few_out)
    answered[:, QUARTERS * MAIN :, :] = back.reshape(sources, few, part).astype(BF)


def shared_body(normed, w, out):
    devices, three, features = w.shape
    few = three // 3
    parts = [w[:, i * few : (i + 1) * few, :].reshape(devices * few, features) for i in range(3)]
    n = normed[...]
    gate = dot_nt(n, parts[0])
    up = dot_nt(n, parts[1])
    hidden = (gate / (1.0 + jnp.exp(-gate)) * up).astype(BF)
    out[...] = dot(hidden, parts[2])


def split_weight(w):
    high = w.astype(BF)
    return high, (w - high.astype(F32)).astype(BF)


def mixers_body(routes, route_weight, main_high, main_low, few_high, few_low):
    rows, top = routes.shape
    few = QUARTERS * EXTRA
    experts = main_high.shape[1] // MAIN
    raw = route_weight[...]
    weights = raw / jnp.sum(raw, axis=1, keepdims=True) * ROUTED_SCALE
    ids = [routes[:, k : k + 1] for k in range(top)]
    hot = [(iota((rows, experts), 1) == ids[k]).astype(F32) for k in range(top)]
    named = sum(hot[1:], hot[0])
    earlier = (iota((rows, rows), 1) < iota((rows, rows), 0)).astype(BF)
    before = dot(earlier, named.astype(BF))
    ranks = [jnp.sum(before * h, axis=1, keepdims=True).astype(jnp.int32) for h in hot]
    spot = iota((rows, experts * MAIN), 1)
    main = jnp.zeros((rows, experts * MAIN), F32)
    for k in range(top):
        target = jnp.where(ranks[k] < MAIN, ids[k] * MAIN + ranks[k], -1)
        main = jnp.where(spot == target, weights[:, k : k + 1], main)
    main_high[...], main_low[...] = split_weight(main)
    spot = iota((rows, experts * few), 1)
    for q in range(QUARTERS):
        pick = jnp.zeros((rows, experts * few), F32)
        for k in range(top):
            slot = ids[k] * few + q * EXTRA + ranks[k] - MAIN
            slot = jnp.where(ranks[k] < MAIN, -1, slot)
            pick = jnp.where(spot == slot, weights[:, k : k + 1], pick)
        few_high[q], few_low[q] = split_weight(pick)


def combine_body(returned, main_high, main_low, few_high, few_low, shared_hbm, mixed, shared, sem):
    fetch = pltpu.make_async_copy(shared_hbm, shared, sem)
    fetch.start()
    experts = returned.shape[0]
    part = returned.shape[2]
    few = QUARTERS * EXTRA
    tail = returned[:, QUARTERS * MAIN :, :].astype(F32).reshape(experts * few, part).astype(BF)
    for q in range(QUARTERS):
        x = returned[:, q * MAIN : (q + 1) * MAIN, :].reshape(experts * MAIN, part)
        routed = dot(main_high[...], x) + dot(main_low[...], x)
        routed = routed + dot(few_high[q], tail) + dot(few_low[q], tail)
        if q == 0:
            fetch.wait()
        at = slice(q * part, (q + 1) * part)
        mixed[:, at] = (shared[:, at] + routed).astype(BF)


def swapped(array, axis, other):
    pairs = [(i, i ^ other) for i in range(lax.axis_size(axis))]
    return lax.ppermute(array, axis, pairs) if other else array


def place_of(index, other, block):
    return pl.ds(pl.multiple_of((index[0] ^ other) * block, block), block)


def few_body(index, *refs):
    stacks, out = refs[:-1], refs[-1]
    side, rows, block = stacks[0].shape
    for j, stack in enumerate(stacks):
        for k in range(side):
            out[:, place_of(index, j * side + k, block)] = stack[k, rows - out.shape[0] :, :]


def split_body(index, shr, *refs):
    outs = refs[-6:]
    side = (len(refs) - 6) // 2
    first, second = refs[:side], refs[side : 2 * side]
    gate, up, down = outs[:3]
    rows = gate.shape[1]
    half = rows // 2
    block = first[0].shape[2]
    for i in range(side):
        for j in range(side):
            at = place_of(index, i * side + j, block)
            gate[0, :, at] = first[i][j, :rows, :]
            up[0, :half, at] = first[i][j, rows : rows + half, :]
            up[0, half:, at] = second[j][i, :half, :]
            down[0, :, at] = second[j][i, half : half + rows, :]
    for i, ref in enumerate(outs[3:]):
        ref[...] = shr[i * ref.shape[0] : (i + 1) * ref.shape[0], :]


def step(tokens, gain, ex_gate, ex_up, ex_down, sh_gate, sh_up, sh_down, routes, route_weight):
    rows, features = tokens.shape
    hidden, block = ex_gate.shape[1:]
    few = sh_gate.shape[0]
    experts = lax.axis_size(TP)
    part = features // QUARTERS
    shape = jax.ShapeDtypeStruct

    args = (gain[None, :], ex_gate, ex_up, ex_down, sh_gate, sh_up, sh_down)
    cut = 3 * hidden // 2
    out = (shape((2 * cut, block), BF), shape((cut + 3 * few, block), BF), shape((cut, block), BF))
    routed_w, first_w, second_w = call(fold_body, out, args, 10**6)
    over_z = lax.all_gather(routed_w, "tp_0", axis=0, tiled=False)
    size = MAIN * QUARTERS + EXTRA * QUARTERS
    out = (shape((experts, size, part), BF), shape((rows, features), BF))
    flops = 2 * rows * features * experts * (MAIN + EXTRA)
    outgoing, normed = call(place_body, out, (tokens, routes.T), flops)
    arrived = lax.all_to_all(outgoing, PLANE, 0, 0, tiled=True)
    side = lax.axis_size("x")
    first = jnp.stack([first_w, swapped(first_w, "x", 1)])
    second = jnp.stack([second_w, swapped(second_w, "y", 1)])
    first = jnp.concatenate([first, swapped(first, "x", 2)])
    second = jnp.concatenate([second, swapped(second, "y", 2)])
    firsts = [swapped(first, "y", k) for k in range(side)]
    index = lax.axis_index(FS).astype(jnp.int32).reshape(1)
    scalar = [pl.BlockSpec(memory_space=pltpu.SMEM)]
    out = (shape((3 * few, features), BF),)
    specs = scalar + [whole(first.shape)] * side
    (shr,) = call(few_body, out, (index, *firsts), 10**6, None, specs)
    shared_w = lax.all_gather(shr, TP, axis=0, tiled=False)
    seconds = [swapped(second, "x", k) for k in range(side)]
    out = (shape((1, hidden, features), BF),) * 3 + (shape((few, features), BF),) * 3
    specs = scalar + [whole(shr.shape)] + [whole(first.shape)] * side + [whole(second.shape)] * side
    outs = call(split_body, out, (index, shr, *firsts, *seconds), 10**7, None, specs)
    expert_w = lax.all_to_all(over_z, FS, 0, 0, tiled=True)
    n = experts * MAIN
    m = experts * EXTRA
    out = shape(outgoing.shape, BF)
    answered = pl.pallas_call(
        expert_body,
        out_shape=out,
        in_specs=[whole(arrived.shape), whole(expert_w.shape)],
        out_specs=whole(out.shape),
        scratch_shapes=[
            pltpu.VMEM((n, 2 * hidden), F32),
            pltpu.VMEM((m, 2 * hidden), F32),
            pltpu.VMEM((n, hidden), BF),
            pltpu.VMEM((m, hidden), BF),
        ],
        cost_estimate=pl.CostEstimate(
            flops=6 * (n + m) * hidden * features, bytes_accessed=8 * 10**6, transcendentals=0
        ),
        compiler_params=pltpu.CompilerParams(vmem_limit_bytes=GRANT),
        name="experts",
    )(arrived, expert_w)
    returned = lax.all_to_all(answered, PLANE, 0, 0, tiled=True)
    out = (shape((rows, n), BF),) * 2 + (shape((QUARTERS, rows, m * QUARTERS), BF),) * 2
    mixers = call(mixers_body, out, (routes, route_weight), 10**7)
    out = (shape((rows, features), F32),)
    (shared,) = call(shared_body, out, (normed, shared_w), 6 * rows * features * few * experts)
    out = (shape((rows, features), BF),)
    args = (returned, *mixers, shared)
    specs = [whole(a.shape) for a in args[:-1]] + [pl.BlockSpec(memory_space=pltpu.HBM)]
    scratch = [pltpu.VMEM((rows, features), F32), pltpu.SemaphoreType.DMA(())]
    (mixed,) = call(
        combine_body, out, args, 4 * rows * features * (n + m), GRANT, specs, (), scratch
    )
    return (mixed, *outs)


def solution(mesh):
    split = Mesh(mesh.devices.reshape(4, 4, 16, 2), FS_TP)
    in_specs = (
        P(FS_TP, None),
        P(FS),
        P(TP, None, FS),
        P(TP, None, FS),
        P(TP, None, FS),
        P(TP, FS),
        P(TP, FS),
        P(TP, FS),
        P(FS_TP, None),
        P(FS_TP, None),
    )
    out_specs = (
        P(FS_TP, None),
        P(TP, None, None),
        P(TP, None, None),
        P(TP, None, None),
        P(TP, None),
        P(TP, None),
        P(TP, None),
    )
    return jax.shard_map(step, mesh=split, in_specs=in_specs, out_specs=out_specs, check_vma=False)
```
